32 devices in a mesh: sp: 16 (over z, y, x), tp: 2 (over core).
Axes of the slice: x: 2, y: 2, z: 4, core: 2. Of those that a mesh axis runs over, the one named last changes fastest.
Arguments:
- stream: bfloat16 [6144, 2048], P('sp'), may hold values from -40 to 40
- query_rows: bfloat16 [6144, 1024], P('sp', 'tp'), may hold values from -10 to 10
- key_rows: bfloat16 [6144, 256], P('sp'), may hold values from -10 to 10
- value_rows: bfloat16 [6144, 256], P('sp'), may hold values from -6 to 6
- doc_ids: int32 [6144], P('sp'), may hold values from 0 to 7, never falling along the last dimension, each value on 1 to 1536 neighbouring positions
- sink_logit: float32 [8], P('tp'), may hold values from 2 to 7
- out_weight: bfloat16 [1024, 2048], P('tp'), may hold values from -1.5 to 1.5
- norm_gain: float32 [2048], replicated, may hold values from 0.1 to 1.9
- gate_weight: bfloat16 [2048, 5632], P('sp', 'tp'), may hold values from -0.125 to 0.125
- up_weight: bfloat16 [2048, 5632], P('sp', 'tp'), may hold values from -0.125 to 0.125
- down_weight: bfloat16 [5632, 2048], P('tp', 'sp'), may hold values from -0.078125 to 0.078125
Outputs:
- mixed_out: bfloat16 [6144, 2048], P('sp')
The draws below stay inside these ranges and needn't reach their ends.
Inputs may be any that keep to these rules, and one draw needn't show every extreme that they name: `doc_ids`: document numbers never fall along the sequence; each document has 1 to 1536 positions.
All inputs are finite; a program needn't handle non-finite values.
Results may differ from the reference program's by a relative error of at most 0.009.
Values may be sent and summed in bfloat16 or wider, within the bound.
No kernel may reach another device: no remote copies, remote signals or barrier semaphores. Data moves between devices by JAX's collectives and lax.ppermute only.
A program may use at most 128 MiB of HBM per device.

```python
import math
import jax
import jax.numpy as jnp
import numpy as np
from jax import lax

D = 2048
FF = 5632
HEADS = 8
KVH = 2
HD = 128
WIN = 128
TOK_DEV = 384
TOKENS = 6144
DOCS = 8
DOC_MOST = 1536
N_TP = 2


def draw_stream(key, part):
    first_key, second_key = jax.random.split(key, 2)
    column_scale = 3.0 ** (jnp.arange(D, dtype=jnp.float32) / D)
    base = jnp.clip(jax.random.normal(first_key, (TOKENS, D), jnp.float32), -6.0, 6.0)
    row_scale = jnp.exp(jax.random.uniform(second_key, (TOKENS, 1), jnp.float32, -0.7, 0.7))
    values = base * row_scale * column_scale[None, :]
    return values.astype(jnp.bfloat16)


def draw_query_rows(key, part):
    values = jnp.clip(jax.random.normal(jax.random.fold_in(key, 1), (TOKENS, HEADS * HD), jnp.float32), -6.0, 6.0)
    return values.astype(jnp.bfloat16)


def draw_key_rows(key, part):
    values = jnp.clip(jax.random.normal(jax.random.fold_in(key, 2), (TOKENS, KVH * HD), jnp.float32), -6.0, 6.0)
    return values.astype(jnp.bfloat16)


def block_levels(stream_key, dims, pieces, least, largest):
    def one(dim, blocks):
        heights = jax.random.uniform(jax.random.fold_in(jax.random.fold_in(stream_key, 6), dim), (blocks,), jnp.float32, least / len(pieces), largest / len(pieces))
        return jnp.repeat(jnp.exp(heights), dims[dim] // blocks).reshape((-1,) + (1,) * (len(dims) - dim - 1))

    loudness = one(*pieces[0])
    for cut in pieces[1:]:
        loudness = loudness * one(*cut)
    return loudness


def profile(count, total, reach, slope):
    portions = [(1 << 20) // math.isqrt(rank ** slope) + 1 for rank in range(2, count + 1)]
    surplus, holding = total - reach - (count - 1), [1] * (count - 1)
    while surplus > 0:
        free = [i for i in range(count - 1) if holding[i] < reach]
        whole, remaining = sum([portions[i] for i in free]), surplus
        for i in free:
            more = min(reach - holding[i], max(1, remaining * portions[i] // whole), surplus)
            holding[i] = holding[i] + more
            surplus = surplus - more
    return np.array([reach] + holding)


def uneven_parts(rng, count, total, limit, skew):
    if count == 2:
        one = jax.random.randint(rng, (), max(1, total - limit), min(limit, total - 1) + 1)
        return jnp.stack([one, total - one])
    lengths = jnp.asarray(profile(count, total, limit, skew), jnp.int32)
    couples = (count - 1) // 2
    source_of, sink = lengths[1:1 + 2 * couples:2], lengths[2:2 + 2 * couples:2]
    room = jnp.minimum(source_of - 1, limit - sink)
    passed = jax.random.randint(jax.random.fold_in(rng, 1), (couples,), 0, 1 << 20) % (room + 1)
    lengths = lengths.at[1:1 + 2 * couples:2].set(source_of - passed).at[2:2 + 2 * couples:2].set(sink + passed)
    return lengths[jax.random.permutation(jax.random.fold_in(rng, 2), count)]


def noise(own_key, shape, scale, bound, cuts=(), kind=jnp.bfloat16):
    level = block_levels(own_key, shape, cuts, -0.22, 0.18) if cuts else 1.0
    entries = jax.random.normal(own_key, shape, jnp.float32) * scale * level
    return jnp.minimum(jnp.maximum(entries, -bound), bound).astype(kind)


def setup_inputs(seed: int = 0) -> dict:
    splits = jax.random.split(jax.random.key(seed), 12)
    return {
        "stream": draw_stream(jax.random.fold_in(splits[11], 71), 0),
        "query_rows": draw_query_rows(jax.random.fold_in(splits[11], 71), 0),
        "key_rows": draw_key_rows(jax.random.fold_in(splits[11], 71), 0),
        "value_rows": noise(splits[3], (TOKENS, KVH * HD), 1.0, 6.0, ((0, 16),)),
        "doc_ids": jnp.searchsorted(jnp.cumsum(uneven_parts(splits[4], DOCS, TOKENS, DOC_MOST, 1)), jnp.arange(TOKENS), side="right").astype(jnp.int32),
        "sink_logit": jnp.clip(2.0 + 5.0 * jax.random.uniform(splits[5], (HEADS,), jnp.float32) ** block_levels(splits[5], (HEADS,), ((0, 2),), -0.2, 0.2), 2.0, 7.0),
        "out_weight": noise(splits[6], (HEADS * HD, D), (HEADS * HD // 64) ** -0.5, 1.5, ((0, 2),)),
        "norm_gain": jnp.clip(1.0 + 0.18 * jax.random.normal(splits[7], (D,), jnp.float32), 0.1, 1.9),
        "gate_weight": noise(splits[8], (D, FF), D ** -0.5, 0.125, ((0, 16), (1, 2))),
        "up_weight": noise(splits[9], (D, FF), D ** -0.5, 0.125, ((0, 16), (1, 2))),
        "down_weight": noise(splits[10], (FF, D), FF ** -0.5, 0.078125, ((0, 2), (1, 16))),
    }


norm_eps = 1e-06
masked_low = -1e+30

def reference(stream, query_rows, key_rows, value_rows, doc_ids, sink_logit, out_weight, norm_gain, gate_weight, up_weight, down_weight):
    seq_total = stream.shape[0]
    group_share = HEADS // KVH
    keys_pad = jnp.pad(key_rows, ((WIN, WIN), (0, 0)))
    values_pad = jnp.pad(value_rows, ((WIN, WIN), (0, 0)))
    docs_pad = jnp.pad(doc_ids, (WIN, WIN))
    head_block = HEADS * HD // N_TP
    ff_block = FF // N_TP
    span = TOK_DEV + 2 * WIN

    def one_block(block_id):
        begin_at = (block_id * TOK_DEV).astype(jnp.int32)
        queries = lax.dynamic_slice_in_dim(query_rows, begin_at, TOK_DEV, 0).astype(jnp.float32).reshape(TOK_DEV, KVH, group_share, HD)
        keys_grid = lax.dynamic_slice_in_dim(keys_pad, begin_at, span, 0).astype(jnp.float32).reshape(span, KVH, HD)
        values_grid = lax.dynamic_slice_in_dim(values_pad, begin_at, span, 0).astype(jnp.float32).reshape(span, KVH, HD)
        docs_here = lax.dynamic_slice_in_dim(doc_ids, begin_at, TOK_DEV, 0)
        docs_wide = lax.dynamic_slice_in_dim(docs_pad, begin_at, span, 0)
        query_pos = begin_at + jnp.arange(TOK_DEV, dtype=jnp.int32)
        key_pos = begin_at - WIN + jnp.arange(span, dtype=jnp.int32)
        allowed = (jnp.abs(query_pos[:, None] - key_pos[None, :]) <= WIN) & (key_pos[None, :] >= 0) & (key_pos[None, :] < seq_total) & (docs_here[:, None] == docs_wide[None, :])
        scores = jnp.einsum('qgrd,kgd->grqk', queries, keys_grid) * HD ** (-0.5)
        masked = jnp.where(allowed[None, None], scores, masked_low)
        sinks = sink_logit.astype(jnp.float32).reshape(KVH, group_share, 1, 1)
        peak = jnp.maximum(lax.optimization_barrier(jnp.max(masked, axis=-1, keepdims=True)), sinks)
        lifted = jnp.where(allowed[None, None], jnp.exp(masked - peak), 0.0)
        denom = lax.optimization_barrier(jnp.sum(lifted, axis=-1, keepdims=True)) + jnp.exp(sinks - peak)
        probs = (lifted / denom).astype(jnp.bfloat16)
        attended = jnp.einsum('grqk,kgd->qgrd', probs.astype(jnp.float32), values_grid)
        attended = attended.astype(jnp.bfloat16).reshape(TOK_DEV, HEADS * HD)
        branch_sum = jnp.zeros((TOK_DEV, D), jnp.float32)
        for part_id in range(N_TP):
            term = jnp.dot(attended[:, part_id * head_block:(part_id + 1) * head_block], out_weight[part_id * head_block:(part_id + 1) * head_block], preferred_element_type=jnp.float32)
            branch_sum = branch_sum + lax.optimization_barrier(term.astype(jnp.bfloat16)).astype(jnp.float32)
        branch = branch_sum.astype(jnp.bfloat16)
        stream_here = lax.dynamic_slice_in_dim(stream, begin_at, TOK_DEV, 0)
        carried = (stream_here.astype(jnp.float32) + branch.astype(jnp.float32)).astype(jnp.bfloat16)
        carried_f = carried.astype(jnp.float32)
        normed = (carried_f * lax.rsqrt(lax.optimization_barrier(jnp.mean(carried_f * carried_f, axis=1, keepdims=True)) + norm_eps) * norm_gain.astype(jnp.float32)).astype(jnp.bfloat16)
        gate_acc = jnp.dot(normed, gate_weight, preferred_element_type=jnp.float32)
        up_acc = jnp.dot(normed, up_weight, preferred_element_type=jnp.float32)
        hidden = (jax.nn.silu(gate_acc) * up_acc).astype(jnp.bfloat16)
        feed_sum = jnp.zeros((TOK_DEV, D), jnp.float32)
        for part_id in range(N_TP):
            term = jnp.dot(hidden[:, part_id * ff_block:(part_id + 1) * ff_block], down_weight[part_id * ff_block:(part_id + 1) * ff_block], preferred_element_type=jnp.float32)
            feed_sum = feed_sum + lax.optimization_barrier(term.astype(jnp.bfloat16)).astype(jnp.float32)
        feed = feed_sum.astype(jnp.bfloat16)
        return (carried_f + 0.5 * feed.astype(jnp.float32)).astype(jnp.bfloat16)
    blocks_all = lax.map(one_block, jnp.arange(seq_total // TOK_DEV, dtype=jnp.int32))
    return blocks_all.reshape(seq_total, D)
```

```python
import jax
import jax.numpy as jnp
from jax import lax
from jax.sharding import PartitionSpec as P

HEADS = 8
KVH = 2
HD = 128
WIN = 128

norm_eps = 1e-06
masked_low = -1e30


AXES = ("t", "f", "tp")


def near_size(count):
    near = 1
    while near * near * 4 <= count and count % (near * 2) == 0:
        near *= 2
    return near


def solution(mesh):
    sp_size, tp_size = mesh.shape["sp"], mesh.shape["tp"]
    near = near_size(sp_size)
    far = sp_size // near
    bits = near.bit_length() - 1
    inner = jax.sharding.Mesh(mesh.devices.reshape(far, near, tp_size), AXES)

    def move(value, where):
        pairs = []
        for t in range(far):
            for f in range(near):
                for p in range(tp_size):
                    to = where(t, f, p)
                    if to is not None:
                        a, b, c = to
                        pairs.append(((t * near + f) * tp_size + p, (a * near + b) * tp_size + c))
        return lax.ppermute(value, AXES, pairs)

    def core_swap(value, j):
        return move(value, lambda t, f, p: (t, f, p ^ j))

    def step_bit(step, p):
        return 1 << ((step + p) % bits)

    def near_swap(value, step):
        return move(value, lambda t, f, p: (t, f ^ step_bit(step, p), p))

    def far_move(value, by):
        return move(value, lambda t, f, p: ((t + by) % far, f, p))

    def halo_place(t, f, p):
        s = t * near + f + (1 if p < tp_size // 2 else -1)
        return (s // near, s % near, p) if 0 <= s < sp_size else None

    def far_gather(chunk, dim):
        got = {0: chunk}
        up, down = chunk, chunk
        for by in range(1, (far - 1) // 2 + 1):
            up, down = far_move(up, 1), far_move(down, -1)
            got[far - by], got[by] = up, down
        if far % 2 == 0:
            half = chunk.shape[dim] // 2
            first = far_move(lax.slice_in_dim(up, 0, half, axis=dim), 1)
            second = far_move(lax.slice_in_dim(down, half, 2 * half, axis=dim), -1)
            got[far // 2] = jnp.concatenate([first, second], axis=dim)
        return [got[i] for i in range(far)]

    def per_device(
        stream,
        query_rows,
        key_rows,
        value_rows,
        doc_ids,
        sink_logit,
        out_weight,
        norm_gain,
        gate_weight,
        up_weight,
        down_weight,
    ):
        rows, width = stream.shape
        rows_here = rows // tp_size
        heads_here = query_rows.shape[1] // HD
        group_share = HEADS // KVH
        groups_here = max(1, heads_here // group_share)
        per_group = heads_here // groups_here
        depth, units = gate_weight.shape
        units_here = units // near
        t_at, f_at, p_at = (lax.axis_index(a) for a in AXES)
        sp_at = t_at * near + f_at
        row_first = p_at * rows_here

        own_kv = jnp.concatenate([key_rows, value_rows], axis=1)
        kv_width = own_kv.shape[1]
        edge = jnp.where(p_at < tp_size // 2, rows - WIN, 0)
        docs_edge = lax.dynamic_slice_in_dim(doc_ids, edge, WIN, 0).astype(jnp.bfloat16)
        docs_row = jnp.broadcast_to(jnp.pad(docs_edge, (0, kv_width - WIN))[None, :], (16, kv_width))
        message = jnp.concatenate([lax.dynamic_slice_in_dim(own_kv, edge, WIN, 0), docs_row], axis=0)
        halo = move(message, halo_place)
        halo_docs = halo[WIN, :WIN].astype(jnp.int32)
        halo_kv = halo[:WIN]

        def rows_of(value, place):
            return lax.dynamic_slice_in_dim(value, place * rows_here, rows_here, 0)

        queries_by = [rows_of(query_rows, p_at)]
        sinks_by, out_by = [sink_logit], [out_weight]
        for j in range(1, tp_size):
            queries_by.append(core_swap(rows_of(query_rows, p_at ^ j), j))
            sinks_by.append(core_swap(sink_logit, j))
            out_by.append(core_swap(out_weight, j))

        def near_exchange(value):
            return lax.all_to_all(value, "f", 0, 0, tiled=False)

        gate_cut = gate_weight.reshape(depth, near, units_here).transpose(1, 0, 2)
        up_cut = up_weight.reshape(depth, near, units_here).transpose(1, 0, 2)
        down_cut = down_weight.reshape(near, units_here, depth)
        gate_mine = near_exchange(gate_cut).reshape(near * depth, units_here)
        up_mine = near_exchange(up_cut).reshape(near * depth, units_here)
        down_mine = near_exchange(down_cut)
        down_mine = down_mine.transpose(1, 0, 2).reshape(units_here, near * depth)
        gate_all = jnp.concatenate(far_gather(gate_mine, 0), axis=0)
        up_all = jnp.concatenate(far_gather(up_mine, 0), axis=0)
        down_all = jnp.concatenate(far_gather(down_mine, 1), axis=1)

        span = rows_here + 2 * WIN
        kv_wide = jnp.concatenate([halo_kv, own_kv, halo_kv], axis=0)
        kv_here = lax.dynamic_slice_in_dim(kv_wide, row_first, span, 0)
        docs_wide = jnp.concatenate([halo_docs, doc_ids, halo_docs])
        docs_keys = lax.dynamic_slice_in_dim(docs_wide, row_first, span, 0)
        docs_here = lax.dynamic_slice_in_dim(doc_ids, row_first, rows_here, 0)
        first_pos = sp_at * rows + row_first
        query_pos = first_pos + jnp.arange(rows_here, dtype=jnp.int32)
        key_pos = first_pos - WIN + jnp.arange(span, dtype=jnp.int32)
        allowed = (
            (jnp.abs(query_pos[:, None] - key_pos[None, :]) <= WIN)
            & (key_pos[None, :] >= 0)
            & (key_pos[None, :] < sp_size * rows)
            & (docs_here[:, None] == docs_keys[None, :])
        )
        branch = jnp.zeros((rows_here, width), jnp.float32)
        for j in range(tp_size):
            group_first = (p_at ^ j) * heads_here // group_share
            keys = lax.dynamic_slice_in_dim(kv_here, group_first * HD, groups_here * HD, 1)
            values = lax.dynamic_slice_in_dim(
                kv_here, (KVH + group_first) * HD, groups_here * HD, 1
            )
            queries = queries_by[j].reshape(rows_here, groups_here, per_group, HD)
            scores = jnp.einsum(
                "qgrd,kgd->grqk",
                queries,
                keys.reshape(span, groups_here, HD),
                preferred_element_type=jnp.float32,
            ) * HD ** (-0.5)
            masked = jnp.where(allowed[None, None], scores, masked_low)
            sinks = sinks_by[j].reshape(groups_here, per_group, 1, 1)
            peak = jnp.maximum(jnp.max(masked, axis=-1, keepdims=True), sinks)
            lifted = jnp.where(allowed[None, None], jnp.exp(masked - peak), 0.0)
            denom = jnp.sum(lifted, axis=-1, keepdims=True) + jnp.exp(sinks - peak)
            probs = (lifted / denom).astype(jnp.bfloat16)
            attended = jnp.einsum(
                "grqk,kgd->qgrd",
                probs,
                values.reshape(span, groups_here, HD),
                preferred_element_type=jnp.float32,
            )
            attended = attended.astype(jnp.bfloat16).reshape(rows_here, heads_here * HD)
            branch = branch + jnp.dot(attended, out_by[j], preferred_element_type=jnp.float32)
        branch = branch.astype(jnp.bfloat16)
        stream_here = rows_of(stream, p_at)
        carried = (stream_here.astype(jnp.float32) + branch.astype(jnp.float32)).astype(jnp.bfloat16)
        carried_f = carried.astype(jnp.float32)
        normed = (
            carried_f
            * lax.rsqrt(jnp.mean(carried_f * carried_f, axis=1, keepdims=True) + norm_eps)
            * norm_gain[None, :]
        ).astype(jnp.bfloat16)
        turn = t_at * near * depth
        normed = lax.dynamic_slice_in_dim(
            jnp.concatenate([normed, normed], axis=1), turn, width, 1
        )

        pieces = [normed]
        for step in range(bits):
            pieces = pieces + [near_swap(x, step) for x in pieces]
        mine = jnp.concatenate(pieces, axis=0)
        blocks = [mine] + [
            jnp.concatenate([core_swap(x, j) for x in pieces], axis=0) for j in range(1, tp_size)
        ]
        normed_all = jnp.concatenate(blocks, axis=0)

        gate_acc = jnp.dot(normed_all, gate_all, preferred_element_type=jnp.float32)
        up_acc = jnp.dot(normed_all, up_all, preferred_element_type=jnp.float32)
        hidden = (jax.nn.silu(gate_acc) * up_acc).astype(jnp.bfloat16)
        terms = jnp.dot(hidden, down_all, preferred_element_type=jnp.float32).astype(jnp.bfloat16)

        block = near * rows_here
        total = terms[:block].astype(jnp.float32)
        for j in range(1, tp_size):
            total = total + core_swap(terms[j * block : (j + 1) * block], j).astype(jnp.float32)
        total = total.astype(jnp.bfloat16)
        for step in reversed(range(bits)):
            cut = (1 << step) * rows_here
            got = near_swap(total[cut:], step)
            total = (total[:cut].astype(jnp.float32) + got.astype(jnp.float32)).astype(jnp.bfloat16)
        feed = lax.dynamic_slice_in_dim(
            jnp.concatenate([total, total], axis=1), (width - turn) % width, width, 1
        )
        mixed = (carried_f + 0.5 * feed.astype(jnp.float32)).astype(jnp.bfloat16)
        by = [mixed] + [core_swap(mixed, j) for j in range(1, tp_size)]
        stacked = jnp.stack(by)
        return jnp.concatenate(
            [
                lax.dynamic_index_in_dim(stacked, p_at ^ q, 0, keepdims=False)
                for q in range(tp_size)
            ],
            axis=0,
        )

    rows_spec = ("t", "f")
    in_specs = (
        P(rows_spec, None),
        P(rows_spec, "tp"),
        P(rows_spec, None),
        P(rows_spec, None),
        P(rows_spec),
        P("tp"),
        P("tp", None),
        P(),
        P(rows_spec, "tp"),
        P(rows_spec, "tp"),
        P("tp", rows_spec),
    )
    return jax.shard_map(
        per_device, mesh=inner, in_specs=in_specs, out_specs=P(rows_spec, None), check_vma=False
    )
```
